32 devices in a mesh: gr: 2 (over x), fs: 8 (over z, y), tp: 2 (over core).
Axes of the slice: x: 2, y: 2, z: 4, core: 2. Of those that a mesh axis runs over, the one named last changes fastest.
Arguments:
- prompt: bfloat16 [3072, 2048], P(('gr', 'fs', 'tp')), may hold values from -6 to 6
- norm_first: float32 [2048], P(('gr', 'fs')), may hold values from 0.1 to 1.9
- gate_first: float32 [2048, 5632], P(('gr', 'fs'), 'tp'), may hold values from -6 to 6
- up_first: float32 [2048, 5632], P(('gr', 'fs'), 'tp'), may hold values from -6 to 6
- down_first: float32 [2048, 5632], P(('gr', 'fs'), 'tp'), may hold values from -6 to 6
- norm_second: float32 [2048], P(('gr', 'fs')), may hold values from 0.1 to 1.9
- gate_second: float32 [2048, 5632], P(('gr', 'fs'), 'tp'), may hold values from -6 to 6
- up_second: float32 [2048, 5632], P(('gr', 'fs'), 'tp'), may hold values from -6 to 6
- down_second: float32 [2048, 5632], P(('gr', 'fs'), 'tp'), may hold values from -6 to 6
Outputs:
- served_gate_first: bfloat16 [2048, 5632], P(None, 'fs')
- served_up_first: bfloat16 [2048, 5632], P(None, 'fs')
- served_down_first: bfloat16 [2048, 5632], P(None, 'fs')
- served_gate_second: bfloat16 [2048, 5632], P(None, 'fs')
- served_up_second: bfloat16 [2048, 5632], P(None, 'fs')
- served_down_second: bfloat16 [2048, 5632], P(None, 'fs')
- result: bfloat16 [3072, 2048], P(('gr', 'fs', 'tp'))
The draws below stay inside these ranges and needn't reach their ends.
All inputs are finite; a program needn't handle non-finite values.
Results may differ from the reference program's by a relative error of at most 0.015.
Values may be sent and summed in bfloat16 or wider, within the bound.
No kernel may reach another device: no remote copies, remote signals or barrier semaphores. Data moves between devices by JAX's collectives and lax.ppermute only.
A program may use at most 128 MiB of HBM per device.

```python
import jax
import jax.numpy as jnp
from jax import lax

D = 2048
FF = 5632
FF_BLK = 704
TOKENS = 3072


def block_scale(key, shape, cuts, least, high):
    factor_of = 1.0
    for axis_at, parts in cuts:
        heights = jax.random.uniform(jax.random.fold_in(jax.random.fold_in(key, 6), axis_at), (parts,), jnp.float32, least / len(cuts), high / len(cuts))
        factor_of = factor_of * jnp.repeat(jnp.exp(heights), shape[axis_at] // parts).reshape((-1,) + (1,) * (len(shape) - 1 - axis_at))
    return factor_of


def scatter_about(stream_key, extent, spread, most, pieces=(), kind=jnp.bfloat16):
    level = block_scale(stream_key, extent, pieces, -0.22, 0.18) if pieces else 1.0
    drawn = jax.random.normal(stream_key, extent, jnp.float32) * spread * level
    return jnp.minimum(jnp.maximum(drawn, -most), most).astype(kind)


def setup_inputs(seed: int = 0) -> dict:
    seeds = jax.random.split(jax.random.key(seed), 10)
    prompt = scatter_about(seeds[0], (TOKENS, D), 1.0, 6.0, ((0, 32),))
    norm_first = jnp.clip(1.0 + 0.18 * jax.random.normal(seeds[1], (D,), jnp.float32), 0.1, 1.9)
    gate_first = scatter_about(seeds[2], (D, FF), 1.0, 6.0, ((0, 16), (1, 2)), jnp.float32)
    up_first = scatter_about(seeds[3], (D, FF), 1.0, 6.0, ((0, 16), (1, 2)), jnp.float32)
    down_first = scatter_about(seeds[4], (D, FF), 1.0, 6.0, ((0, 16), (1, 2)), jnp.float32)
    norm_second = jnp.clip(1.0 + 0.18 * jax.random.normal(seeds[5], (D,), jnp.float32), 0.1, 1.9)
    gate_second = scatter_about(seeds[6], (D, FF), 1.0, 6.0, ((0, 16), (1, 2)), jnp.float32)
    up_second = scatter_about(seeds[7], (D, FF), 1.0, 6.0, ((0, 16), (1, 2)), jnp.float32)
    down_second = scatter_about(seeds[8], (D, FF), 1.0, 6.0, ((0, 16), (1, 2)), jnp.float32)
    return dict(prompt=prompt, norm_first=norm_first, gate_first=gate_first, up_first=up_first, down_first=down_first, norm_second=norm_second, gate_second=gate_second, up_second=up_second, down_second=down_second)


EPS = 1e-06

def fold_rows(gain, weight):
    return (gain[:, None] * weight).astype(jnp.bfloat16)

def half_step(residual, gate_weight, up_weight, down_weight):
    resid_f = residual.astype(jnp.float32)
    normed = (resid_f * lax.rsqrt(lax.optimization_barrier(jnp.mean(resid_f * resid_f, axis=-1, keepdims=True)) + EPS)).astype(jnp.bfloat16)
    gate_pre = jnp.dot(normed, gate_weight, preferred_element_type=jnp.float32) * D ** (-0.5)
    up_pre = jnp.dot(normed, up_weight, preferred_element_type=jnp.float32) * D ** (-0.5)
    hidden = (jax.nn.silu(gate_pre) * up_pre).astype(jnp.bfloat16)

    def add_block(running, block_index):
        offset = block_index * FF_BLK
        hid_block = lax.dynamic_slice_in_dim(hidden, offset, FF_BLK, 1)
        down_block = lax.dynamic_slice_in_dim(down_weight, offset, FF_BLK, 1)
        partial_sum = lax.dot_general(hid_block, down_block, (((1,), (1,)), ((), ())), preferred_element_type=jnp.float32) * FF ** (-0.5)
        partial_sum = lax.optimization_barrier(partial_sum.astype(jnp.bfloat16)).astype(jnp.float32)
        return (running + partial_sum, None)
    start_sum = jnp.zeros((residual.shape[0], D), jnp.float32)
    branch, _ = lax.scan(add_block, start_sum, jnp.arange(FF // FF_BLK, dtype=jnp.int32))
    return (resid_f + 0.5 * branch).astype(jnp.bfloat16)

def reference(prompt, norm_first, gate_first, up_first, down_first, norm_second, gate_second, up_second, down_second):
    served_gate_first = fold_rows(norm_first, gate_first)
    served_up_first = fold_rows(norm_first, up_first)
    served_down_first = down_first.astype(jnp.bfloat16)
    served_gate_second = fold_rows(norm_second, gate_second)
    served_up_second = fold_rows(norm_second, up_second)
    served_down_second = down_second.astype(jnp.bfloat16)
    middle = half_step(prompt, served_gate_first, served_up_first, served_down_first)
    result = half_step(middle, served_gate_second, served_up_second, served_down_second)
    return (served_gate_first, served_up_first, served_down_first, served_gate_second, served_up_second, served_down_second, result)
```

```python
import jax
import jax.numpy as jnp
from jax import lax
from jax.experimental import pallas as pl
from jax.experimental.pallas import tpu as pltpu
from jax.sharding import PartitionSpec as P

EPS = 1e-06


def pack_pieces(gain, gate, up, down, blocks, splits):
    rows, cols = gate.shape
    width = cols // blocks
    sub = rows // splits
    count = blocks * splits
    matrices = 3

    def body(gain_ref, gate_ref, up_ref, down_ref, out_ref):
        me = lax.axis_index("fs")
        scale = gain_ref[...]
        for index, ref in enumerate((gate_ref, up_ref, down_ref)):
            for h in range(splits):
                here = slice(h * sub, (h + 1) * sub)
                part = ref[here, :]
                if index < 2:
                    part = scale[here] * part
                part = part.astype(jnp.bfloat16)
                for j in range(blocks):
                    slot = lax.rem(j * splits + h - me + count, count)
                    out_ref[slot, index] = part[:, j * width : (j + 1) * width]

    return pl.pallas_call(
        body,
        out_shape=jax.ShapeDtypeStruct((count, matrices, sub, width), jnp.bfloat16),
        name="pack_pieces",
    )(gain[:, None], gate, up, down)


def assemble(spread_pieces, fs_size, gr_size, tp_size):
    flat = []
    places = []
    for a in range(gr_size):
        own, stacks = spread_pieces[a]
        for k in range(fs_size):
            places.append((a, 0, k, len(flat), None))
            flat.append(own[k])
        for b in range(1, tp_size):
            for k in range(fs_size):
                places.append((a, b, k, len(flat), k))
            flat.append(stacks[b - 1])
    matrices, sub, width = flat[0].shape
    total = gr_size * fs_size * tp_size * sub
    count = len(flat)

    def body(*refs):
        ins = refs[:count]
        outs = refs[count : count + matrices]
        sem = refs[count + matrices]
        g = lax.axis_index("gr")
        f = lax.axis_index("fs")
        t = lax.axis_index("tp")
        block = lax.rem(f, fs_size // tp_size)
        copies = []
        for a, b, k, which, at in places:
            src_g = lax.rem(g - a + gr_size, gr_size)
            h = lax.rem(t - b + tp_size, tp_size)
            src_f = lax.rem(block * tp_size + h - k + fs_size, fs_size)
            row = pl.multiple_of(((src_g * fs_size + src_f) * tp_size + h) * sub, sub)
            for i in range(matrices):
                src = ins[which].at[i] if at is None else ins[which].at[at, i]
                copy = pltpu.make_async_copy(src, outs[i].at[pl.ds(row, sub), :], sem)
                copy.start()
                copies.append(copy)
        for copy in copies:
            copy.wait()

    return pl.pallas_call(
        body,
        in_specs=[pl.BlockSpec(memory_space=pltpu.VMEM)] * count,
        out_specs=[pl.BlockSpec(memory_space=pl.ANY)] * matrices,
        out_shape=[jax.ShapeDtypeStruct((total, width), jnp.bfloat16)] * matrices,
        scratch_shapes=[pltpu.SemaphoreType.DMA],
        name="assemble",
    )(*flat)


def shift(value, axis, size, by):
    return lax.ppermute(value, axis, [(i, (i + by) % size) for i in range(size)])


def first_stage(packed, fs_size, tp_size):
    blocks = fs_size // tp_size
    got = []
    for k in range(fs_size):
        pairs = []
        for f in range(fs_size):
            for t in range(tp_size):
                m = (f + k) % fs_size
                dest = (t * blocks + m // tp_size) * tp_size + m % tp_size
                pairs.append((f * tp_size + t, dest))
        got.append(lax.ppermute(packed[k], ("fs", "tp"), pairs))
    return got


def across(got, gr_size):
    return [got] + [[shift(p, "gr", gr_size, a) for p in got] for a in range(1, gr_size)]


def to_cores(parts, tp_size):
    spread_pieces = []
    for part in parts:
        stacked = jnp.stack(part)
        spread_pieces.append((part, [shift(stacked, "tp", tp_size, b) for b in range(1, tp_size)]))
    return spread_pieces


def partial_sums(tokens_in, weights, in_scale, out_scale):
    gate_weight, up_weight, down_weight = weights
    gate_pre = jnp.dot(tokens_in, gate_weight, preferred_element_type=jnp.float32) * in_scale
    up_pre = jnp.dot(tokens_in, up_weight, preferred_element_type=jnp.float32) * in_scale
    hidden = (jax.nn.silu(gate_pre) * up_pre).astype(jnp.bfloat16)
    return (
        lax.dot_general(
            hidden, down_weight, (((1,), (1,)), ((), ())), preferred_element_type=jnp.float32
        )
        * out_scale
    ).astype(jnp.bfloat16)


def add_branch(residual, partial):
    branch = lax.psum_scatter(partial, "fs", scatter_dimension=0, tiled=True)
    return (residual.astype(jnp.float32) + 0.5 * branch.astype(jnp.float32)).astype(jnp.bfloat16)


def gather_normed(residual):
    resid_f = residual.astype(jnp.float32)
    normed = (
        resid_f * lax.rsqrt(jnp.mean(resid_f * resid_f, axis=-1, keepdims=True) + EPS)
    ).astype(jnp.bfloat16)
    return lax.all_gather(normed, "fs", axis=0, tiled=True)


def solution(mesh):
    gr_size = mesh.shape["gr"]
    fs_size = mesh.shape["fs"]
    tp_size = mesh.shape["tp"]
    blocks = fs_size // tp_size

    def on_device(
        prompt,
        norm_first,
        gate_first,
        up_first,
        down_first,
        norm_second,
        gate_second,
        up_second,
        down_second,
    ):
        width = gate_first.shape[1] * tp_size
        in_scale = prompt.shape[1] ** (-0.5)
        out_scale = width ** (-0.5)
        packed_first = pack_pieces(norm_first, gate_first, up_first, down_first, blocks, tp_size)
        got_first = first_stage(packed_first, fs_size, tp_size)
        tokens_first = gather_normed(prompt)
        across_first = across(got_first, gr_size)
        served_first = assemble(to_cores(across_first, tp_size), fs_size, gr_size, tp_size)
        got_first, norm_second = lax.optimization_barrier((got_first, norm_second))
        packed_second = pack_pieces(
            norm_second, gate_second, up_second, down_second, blocks, tp_size
        )
        got_second = first_stage(packed_second, fs_size, tp_size)
        partial = partial_sums(tokens_first, served_first, in_scale, out_scale)
        partial, got_second = lax.optimization_barrier((partial, got_second))
        middle = add_branch(prompt, partial)
        across_second = across(got_second, gr_size)
        middle, across_second = lax.optimization_barrier((middle, across_second))
        tokens_second = gather_normed(middle)
        served_second = assemble(to_cores(across_second, tp_size), fs_size, gr_size, tp_size)
        result = add_branch(middle, partial_sums(tokens_second, served_second, in_scale, out_scale))
        return (*served_first, *served_second, result)

    rows = ("gr", "fs")
    weight = P(rows, "tp")
    tokens = P(("gr", "fs", "tp"), None)
    half = (P(rows), weight, weight, weight)
    return jax.shard_map(
        on_device,
        mesh=mesh,
        in_specs=(tokens, *half, *half),
        out_specs=(*([P(None, "fs")] * 6), tokens),
        check_vma=False,
    )
```

```python
import jax
import jax.numpy as jnp
from jax import lax
from jax.experimental import pallas as pl
from jax.experimental.pallas import tpu as pltpu
from jax.sharding import PartitionSpec as P

EPS = 1e-06


def pack_pieces(gain, gate, up, down, blocks, splits):
    rows, cols = gate.shape
    width = cols // blocks
    sub = rows // splits
    count = blocks * splits
    matrices = 3

    def body(gain_ref, gate_ref, up_ref, down_ref, out_ref):
        me = lax.axis_index("fs")
        scale = gain_ref[...]
        for index, ref in enumerate((gate_ref, up_ref, down_ref)):
            for h in range(splits):
                here = slice(h * sub, (h + 1) * sub)
                part = ref[here, :]
                if index < 2:
                    part = scale[here] * part
                part = part.astype(jnp.bfloat16)
                for j in range(blocks):
                    slot = lax.rem(j * splits + h - me + count, count)
                    out_ref[slot, index] = part[:, j * width : (j + 1) * width]

    return pl.pallas_call(
        body,
        out_shape=jax.ShapeDtypeStruct((count, matrices, sub, width), jnp.bfloat16),
        name="pack_pieces",
    )(gain[:, None], gate, up, down)


def assemble(spread_pieces, fs_size, gr_size, tp_size):
    flat = []
    places = []
    for a in range(gr_size):
        own, stacks = spread_pieces[a]
        for k in range(fs_size):
            places.append((a, 0, k, len(flat), None))
            flat.append(own[k])
        for b in range(1, tp_size):
            for k in range(fs_size):
                places.append((a, b, k, len(flat), k))
            flat.append(stacks[b - 1])
    matrices, sub, width = flat[0].shape
    total = gr_size * fs_size * tp_size * sub
    count = len(flat)

    def body(*refs):
        ins = refs[:count]
        outs = refs[count : count + matrices]
        sem = refs[count + matrices]
        g = lax.axis_index("gr")
        f = lax.axis_index("fs")
        t = lax.axis_index("tp")
        block = lax.rem(f, fs_size // tp_size)
        copies = []
        for a, b, k, which, at in places:
            src_g = lax.rem(g - a + gr_size, gr_size)
            h = lax.rem(t - b + tp_size, tp_size)
            src_f = lax.rem(block * tp_size + h - k + fs_size, fs_size)
            row = pl.multiple_of(((src_g * fs_size + src_f) * tp_size + h) * sub, sub)
            for i in range(matrices):
                src = ins[which].at[i] if at is None else ins[which].at[at, i]
                copy = pltpu.make_async_copy(src, outs[i].at[pl.ds(row, sub), :], sem)
                copy.start()
                copies.append(copy)
        for copy in copies:
            copy.wait()

    return pl.pallas_call(
        body,
        in_specs=[pl.BlockSpec(memory_space=pltpu.VMEM)] * count,
        out_specs=[pl.BlockSpec(memory_space=pl.ANY)] * matrices,
        out_shape=[jax.ShapeDtypeStruct((total, width), jnp.bfloat16)] * matrices,
        scratch_shapes=[pltpu.SemaphoreType.DMA],
        name="assemble",
    )(*flat)


def shift(value, axis, size, by):
    return lax.ppermute(value, axis, [(i, (i + by) % size) for i in range(size)])


def first_stage(packed, fs_size, tp_size):
    blocks = fs_size // tp_size
    got = []
    for k in range(fs_size):
        pairs = []
        for f in range(fs_size):
            for t in range(tp_size):
                m = (f + k) % fs_size
                dest = (t * blocks + m // tp_size) * tp_size + m % tp_size
                pairs.append((f * tp_size + t, dest))
        got.append(lax.ppermute(packed[k], ("fs", "tp"), pairs))
    return got


def across(got, gr_size):
    return [got] + [[shift(p, "gr", gr_size, a) for p in got] for a in range(1, gr_size)]


def to_cores(parts, tp_size):
    spread_pieces = []
    for part in parts:
        stacked = jnp.stack(part)
        spread_pieces.append((part, [shift(stacked, "tp", tp_size, b) for b in range(1, tp_size)]))
    return spread_pieces


def partial_sums(tokens_in, weights, in_scale, out_scale):
    gate_weight, up_weight, down_weight = weights
    gate_pre = jnp.dot(tokens_in, gate_weight, preferred_element_type=jnp.float32) * in_scale
    up_pre = jnp.dot(tokens_in, up_weight, preferred_element_type=jnp.float32) * in_scale
    hidden = (jax.nn.silu(gate_pre) * up_pre).astype(jnp.bfloat16)
    return (
        lax.dot_general(
            hidden, down_weight, (((1,), (1,)), ((), ())), preferred_element_type=jnp.float32
        )
        * out_scale
    ).astype(jnp.bfloat16)


def ring_order(size):
    return list(range(0, size, 2)) + list(range(size - 1 - size % 2, 0, -2))


def ring_shift(value, size, by):
    order = ring_order(size)
    pairs = [(order[p], order[(p + by) % size]) for p in range(size)]
    return lax.ppermute(value, "fs", pairs)


def ring_sum(chunk, size, beside):
    up = size // 2
    down = size - 1 - up
    acc_up = chunk(up)
    acc_down = chunk(size - down) if down else None
    total = chunk(0).astype(jnp.float32)
    for step in range(up):
        acc_up = ring_shift(acc_up, size, 1)
        share = slice(len(beside) * step // up, len(beside) * (step + 1) // up)
        acc_up, beside[share] = lax.optimization_barrier((acc_up, beside[share]))
        acc_up = acc_up.astype(jnp.float32)
        if step < down:
            acc_down = ring_shift(acc_down, size, -1).astype(jnp.float32)
        if step < up - 1:
            acc_up = (acc_up + chunk(up - 1 - step).astype(jnp.float32)).astype(jnp.bfloat16)
        if step < down - 1:
            more = chunk(size - down + 1 + step).astype(jnp.float32)
            acc_down = (acc_down + more).astype(jnp.bfloat16)
    total = total + acc_up
    return total + acc_down if down else total


def ring_gather(value, size):
    up = size // 2
    down = size - 1 - up
    got = {0: value}
    from_below = value
    from_above = value
    for step in range(1, up + 1):
        from_below = ring_shift(from_below, size, 1)
        got[size - step] = from_below
        if step <= down:
            from_above = ring_shift(from_above, size, -1)
            got[step] = from_above
    return jnp.concatenate([got[r] for r in range(size)], axis=0)


def add_branch(residual, partial, size, in_ring_order, beside):
    rows = residual.shape[0]
    order = ring_order(size)
    places = jnp.array([order.index(f) for f in range(size)], jnp.int32)
    order = jnp.array(order, jnp.int32)
    place = places[lax.axis_index("fs")]

    def chunk(r):
        if in_ring_order:
            return partial[r * rows : (r + 1) * rows]
        at = order[lax.rem(place + r, size)]
        return lax.dynamic_slice_in_dim(partial, at * rows, rows, 0)

    branch = ring_sum(chunk, size, beside)
    return (residual.astype(jnp.float32) + 0.5 * branch).astype(jnp.bfloat16)


def normed_rows(residual):
    resid_f = residual.astype(jnp.float32)
    return (
        resid_f * lax.rsqrt(jnp.mean(resid_f * resid_f, axis=-1, keepdims=True) + EPS)
    ).astype(jnp.bfloat16)


def solution(mesh):
    gr_size = mesh.shape["gr"]
    fs_size = mesh.shape["fs"]
    tp_size = mesh.shape["tp"]
    blocks = fs_size // tp_size

    def on_device(
        prompt,
        norm_first,
        gate_first,
        up_first,
        down_first,
        norm_second,
        gate_second,
        up_second,
        down_second,
    ):
        width = gate_first.shape[1] * tp_size
        in_scale = prompt.shape[1] ** (-0.5)
        out_scale = width ** (-0.5)
        packed_first = pack_pieces(norm_first, gate_first, up_first, down_first, blocks, tp_size)
        got_first = first_stage(packed_first, fs_size, tp_size)
        tokens_first = lax.all_gather(normed_rows(prompt), "fs", axis=0, tiled=True)
        across_first = across(got_first, gr_size)
        served_first = assemble(to_cores(across_first, tp_size), fs_size, gr_size, tp_size)
        got_first, norm_second = lax.optimization_barrier((got_first, norm_second))
        packed_second = pack_pieces(
            norm_second, gate_second, up_second, down_second, blocks, tp_size
        )
        got_second = first_stage(packed_second, fs_size, tp_size)
        partial = partial_sums(tokens_first, served_first, in_scale, out_scale)
        partial, got_second = lax.optimization_barrier((partial, got_second))
        across_second = across(got_second, gr_size)
        moved = [p for part in across_second[1:] for p in part]
        middle = add_branch(prompt, partial, fs_size, False, moved)
        across_second = [got_second] + [
            moved[i * fs_size : (i + 1) * fs_size] for i in range(gr_size - 1)
        ]
        middle, across_second = lax.optimization_barrier((middle, across_second))
        tokens_second = ring_gather(normed_rows(middle), fs_size)
        served_second = assemble(to_cores(across_second, tp_size), fs_size, gr_size, tp_size)
        turned_first = [w.T for w in served_first]
        tokens_second, turned_first = lax.optimization_barrier((tokens_second, turned_first))
        turned = [w.T for w in served_second]
        partial = partial_sums(tokens_second, served_second, in_scale, out_scale)
        result = add_branch(middle, partial, fs_size, True, turned)
        return (*[w.T for w in turned_first], *[w.T for w in turned], result)

    rows = ("gr", "fs")
    weight = P(rows, "tp")
    tokens = P(("gr", "fs", "tp"), None)
    half = (P(rows), weight, weight, weight)
    return jax.shard_map(
        on_device,
        mesh=mesh,
        in_specs=(tokens, *half, *half),
        out_specs=(*([P(None, "fs")] * 6), tokens),
        check_vma=False,
    )
```
